32 devices in a mesh: ep: 8 (over z, x), tp: 4 (over y, core).
Axes of the slice: x: 2, y: 2, z: 4, core: 2. Of those that a mesh axis runs over, the one named last changes fastest.
Arguments:
- tokens: bfloat16 [1024, 2048], P('ep', 'tp'), may hold values from -20 to 20
- routing: int32 [1024, 2], P('ep'), may hold values from 0 to 7, all different within a row; in each aligned block of 128 rows (0 to 127, 128 to 255, ...) at most 48 rows name the same one
- gate_weights: bfloat16 [1024, 2], P('ep'), may hold values from 0 to 1, as said below
- cotangent: bfloat16 [1024, 2048], P('ep', 'tp'), may hold values from -3 to 3
- expert_gate: bfloat16 [8, 2048, 3072], P('ep', None, 'tp'), may hold values from -3 to 3
- expert_up: bfloat16 [8, 2048, 3072], P('ep', None, 'tp'), may hold values from -3 to 3
- expert_down: bfloat16 [8, 3072, 2048], P('ep', 'tp'), may hold values from -0.109375 to 0.109375
- router: bfloat16 [2048, 8], replicated, may hold values from -0.125 to 0.125
Outputs:
- token_grad: float32 [1024, 2048], P('ep', 'tp')
- gate_grad: float32 [1024, 2], P('ep')
- gate_proj_grad: bfloat16 [8, 2048, 3072], P('ep', None, 'tp')
- up_proj_grad: bfloat16 [8, 2048, 3072], P('ep', None, 'tp')
- down_proj_grad: bfloat16 [8, 3072, 2048], P('ep', 'tp')
- router_grad: float32 [8, 2048], P('ep', 'tp')
- gate_row_square: float32 [8, 2048], P('ep')
- up_row_square: float32 [8, 2048], P('ep')
- down_row_square: float32 [8, 3072], P('ep', 'tp')
The draws below stay inside these ranges and needn't reach their ends.
Inputs may be any that keep to these rules, and one draw needn't show every extreme that they name: `routing`: each token names 2 different experts. Among the 128 rows of one device no expert is named more than 48 times; some device reaches 48. `gate_weights`: each row is positive and sums to one up to rounding.
All inputs are finite; a program needn't handle non-finite values.
Results may differ from the reference program's by a relative error of at most 0.015.
Values may be sent and summed in bfloat16 or wider, within the bound.
No kernel may reach another device: no remote copies, remote signals or barrier semaphores. Data moves between devices by JAX's collectives and lax.ppermute only.
A program may use at most 64 MiB of HBM per device.

```python
import math
import jax
import jax.numpy as jnp
import numpy as np
from jax import lax

D = 2048
FF = 3072
TOP = 2
TOK_DEV = 128
EXPERTS = 8
CAP = 48
TOKENS = 1024
N_EP = 8
N_TP = 4


def feature_scale(key, length, spread):
    place = jnp.arange(length, dtype=jnp.float32) / length
    jitter = jax.random.uniform(key, (length,), jnp.float32, -0.5, 0.5)
    return jnp.exp(jnp.log(spread) * (place - 0.5) + jitter)


def base_values(key, shape):
    return jnp.clip(jax.random.normal(key, shape, jnp.float32), -5.0, 5.0)


def scaled_matrix(key):
    values = base_values(jax.random.fold_in(key, 21), (EXPERTS, D, FF))
    spread = 3.0
    columns = feature_scale(jax.random.fold_in(key, 22), FF, spread)
    return (values * columns * D ** (-0.5)).astype(jnp.bfloat16)


def draw_tokens(key, part):
    values = base_values(jax.random.fold_in(key, 11), (TOKENS, D))
    columns = feature_scale(jax.random.fold_in(key, 12), D, 3.0)
    return (values * columns).astype(jnp.bfloat16)


def draw_gate_weights(key, part):
    logits = jax.random.uniform(key, (TOKENS, TOP), jnp.float32, -1.5, 1.5)
    return jax.nn.softmax(logits, axis=-1).astype(jnp.bfloat16)


def draw_expert_gate(key, part):
    return scaled_matrix(jax.random.fold_in(key, 31))


def draw_expert_up(key, part):
    return scaled_matrix(jax.random.fold_in(key, 32))


def shard_levels(stream_key, shape, split, least, largest):
    level = 1.0
    for dim, parts in split:
        draws = jax.random.uniform(jax.random.fold_in(jax.random.fold_in(stream_key, 6), dim), (parts,), jnp.float32, least / len(split), largest / len(split))
        level = level * jnp.repeat(jnp.exp(draws), shape[dim] // parts).reshape((-1,) + (1,) * (len(shape) - 1 - dim))
    return level


def assign_block(own_key, own, number, rows, count, top, reach, slope):
    order = jax.random.permutation(own_key, count)
    crowded, common = load_shares(count, rows * top, reach, slope, True), load_shares(count, rows * top, reach, slope, False)
    places = jnp.arange(count)

    def named(lengths, rotation):
        used = int((lengths > 0).sum())
        fixed = max(1, used // 4)
        moved = fixed + (places - fixed + rotation * (used - fixed)) % max(1, count - fixed)
        return jnp.zeros((count,), jnp.int32).at[order[jnp.where(places < fixed, places, moved)]].set(jnp.asarray(lengths, jnp.int32))

    lengths = jnp.where(number % 4 == 0, named(crowded, number // 4), named(common, number - number // 4 - 1))
    mixed = jax.random.permutation(jax.random.fold_in(own, 3), count)
    giver, sink = mixed[0:count // 2 * 2:2], mixed[1:count // 2 * 2:2]
    slack = jnp.minimum(lengths[giver] - 1, reach - lengths[sink]) // 2
    slack = jnp.where((giver == order[0]) | (sink == order[0]) | (lengths[sink] == 0), 0, jnp.maximum(slack, 0))
    moved = jax.random.randint(jax.random.fold_in(own, 4), (count // 2,), 0, 1 << 20) % (slack + 1)
    lengths = lengths.at[giver].add(-moved).at[sink].add(moved)
    items = jnp.searchsorted(jnp.cumsum(lengths), jnp.arange(rows * top), side="right").astype(jnp.int32)
    listing = items.reshape(top, rows).T
    listing = listing[jax.random.permutation(jax.random.fold_in(own, 1), rows)]
    rotation = jax.random.randint(jax.random.fold_in(own, 2), (rows, 1), 0, top)
    return jnp.take_along_axis(listing, (jnp.arange(top)[None, :] + rotation) % top, axis=1)


def load_shares(count, total, reach, slope, full):
    loads = [(1 << 20) // math.isqrt(grade ** slope) + 1 for grade in range(1, count + 1)]
    largest = reach if full else min(reach, max(-(-total // count), total * loads[0] // sum(loads)))
    least = 1 if total - largest >= count - 1 else 0
    counts, rest = [largest] + [least] * (count - 1), total - largest - least * (count - 1)
    while rest > 0:
        free = [i for i in range(1, count) if counts[i] < largest] or [i for i in range(1, count) if counts[i] < reach]
        whole, left = sum([loads[i] for i in free]), rest
        for i in free:
            more = min(reach - counts[i], max(1, left * loads[i] // whole), rest)
            counts[i] = counts[i] + more
            rest = rest - more
    return np.array(counts)


def bell_draw(stream_key, dims, scale, most, pieces=(), held_as=jnp.bfloat16):
    result = scale * jax.random.normal(stream_key, dims, jnp.float32)
    if pieces:
        result = result * shard_levels(stream_key, dims, pieces, -0.22, 0.18)
    return jnp.clip(result, -most, most).astype(held_as)


def setup_inputs(seed: int = 0) -> dict:
    arg_keys = jax.random.split(jax.random.key(seed), 9)
    tokens = draw_tokens(jax.random.fold_in(arg_keys[8], 71), 0)
    routing_keys = jax.random.split(jax.random.fold_in(arg_keys[1], 1), TOKENS // TOK_DEV)
    routing_turns = jax.random.permutation(jax.random.fold_in(arg_keys[1], 3), TOKENS // TOK_DEV)
    routing = jax.vmap(lambda own, number: assign_block(jax.random.fold_in(arg_keys[1], 2), own, number, TOK_DEV, EXPERTS, TOP, CAP, 1))(routing_keys, routing_turns).reshape((TOKENS, TOP))
    gate_weights = draw_gate_weights(jax.random.fold_in(arg_keys[8], 71), 0)
    cotangent = bell_draw(arg_keys[3], (TOKENS, D), 0.5, 3.0, ((0, 8), (1, 4)))
    expert_gate = draw_expert_gate(jax.random.fold_in(arg_keys[8], 71), 0)
    expert_up = draw_expert_up(jax.random.fold_in(arg_keys[8], 71), 0)
    expert_down = bell_draw(arg_keys[6], (EXPERTS, FF, D), FF ** -0.5, 0.109375, ((0, 8), (1, 4)))
    router = bell_draw(arg_keys[7], (D, EXPERTS), D ** -0.5, 0.125)
    return {"tokens": tokens, "routing": routing, "gate_weights": gate_weights, "cotangent": cotangent, "expert_gate": expert_gate, "expert_up": expert_up, "expert_down": expert_down, "router": router}


def reference(tokens, routing, gate_weights, cotangent, expert_gate, expert_up, expert_down, router):
    pair_count = TOK_DEV * TOP
    block_routes = routing.reshape(N_EP, pair_count)
    slot_ids = jnp.arange(CAP, dtype=jnp.int32)
    pair_ids = jnp.arange(pair_count, dtype=jnp.int32)
    block_base = (jnp.arange(N_EP, dtype=jnp.int32) * TOK_DEV)[:, None]
    hidden_local = FF // N_TP

    def one_expert(expert_index):
        hit_mask = (block_routes == expert_index).astype(jnp.int32)
        ranking = (jnp.cumsum(hit_mask, axis=1) - 1).astype(jnp.int32)
        chosen = hit_mask[:, None, :] * (ranking[:, None, :] == slot_ids[None, :, None]).astype(jnp.int32)
        source_pair = jnp.sum(chosen * pair_ids[None, None, :], axis=2).astype(jnp.int32)
        filled = jnp.sum(chosen, axis=2) > 0
        row_index = (block_base + source_pair // TOP).reshape(-1).astype(jnp.int32)
        which_slot = (source_pair % TOP).reshape(-1).astype(jnp.int32)
        live_slot = filled.reshape(-1)
        input_slots = jnp.where(live_slot[:, None], tokens[row_index], jnp.zeros((), jnp.bfloat16))
        tangent_slots = jnp.where(live_slot[:, None], cotangent[row_index], jnp.zeros((), jnp.bfloat16))
        slot_weight = jnp.where(live_slot, gate_weights[row_index, which_slot].astype(jnp.float32), jnp.float32(0.0))
        gate_matrix = expert_gate[expert_index]
        up_matrix = expert_up[expert_index]
        down_matrix = expert_down[expert_index]
        pre_gate = jnp.dot(input_slots, gate_matrix, preferred_element_type=jnp.float32)
        pre_up = jnp.dot(input_slots, up_matrix, preferred_element_type=jnp.float32)
        back_proj = jnp.dot(tangent_slots, down_matrix.T, preferred_element_type=jnp.float32)
        sigmoid_gate = jax.nn.sigmoid(pre_gate)
        active = pre_gate * sigmoid_gate
        hidden = active * pre_up
        slot_gate = jnp.sum(hidden * back_proj, axis=1)
        weight_col = slot_weight[:, None]
        scaled = (weight_col * hidden).astype(jnp.bfloat16)
        hidden_grad = weight_col * back_proj
        gate_pre_grad = (hidden_grad * pre_up * sigmoid_gate * (1.0 + pre_gate * (1.0 - sigmoid_gate))).astype(jnp.bfloat16)
        up_pre_grad = (hidden_grad * active).astype(jnp.bfloat16)
        gate_sum = jnp.dot(input_slots.T, gate_pre_grad, preferred_element_type=jnp.float32)
        up_sum = jnp.dot(input_slots.T, up_pre_grad, preferred_element_type=jnp.float32)
        down_sum = jnp.dot(scaled.T, tangent_slots, preferred_element_type=jnp.float32)
        slot_total = N_EP * CAP
        block_parts = jnp.einsum('snf,dnf->nsd',
                                 gate_pre_grad.astype(jnp.float32).reshape(slot_total, N_TP, hidden_local),
                                 gate_matrix.astype(jnp.float32).reshape(D, N_TP, hidden_local))
        block_parts = block_parts + jnp.einsum('snf,dnf->nsd',
                                               up_pre_grad.astype(jnp.float32).reshape(slot_total, N_TP, hidden_local),
                                               up_matrix.astype(jnp.float32).reshape(D, N_TP, hidden_local))
        rounded = lax.optimization_barrier(block_parts.astype(jnp.bfloat16))
        slot_token = jnp.sum(rounded.astype(jnp.float32), axis=0)
        return (slot_token.reshape(N_EP, CAP, D), slot_gate.reshape(N_EP, CAP),
                gate_sum.astype(jnp.bfloat16), up_sum.astype(jnp.bfloat16), down_sum.astype(jnp.bfloat16),
                jnp.mean(gate_sum * gate_sum, axis=1), jnp.mean(up_sum * up_sum, axis=1),
                jnp.mean(down_sum * down_sum, axis=1))

    results = lax.map(one_expert, jnp.arange(EXPERTS, dtype=jnp.int32))
    slot_token, slot_gate, gate_grads, up_grads, down_grads, gate_square, up_square, down_square = results
    labels = jnp.arange(EXPERTS, dtype=jnp.int32)
    one_hot = (block_routes[:, :, None] == labels[None, None, :]).astype(jnp.int32)
    ranking = (jnp.cumsum(one_hot, axis=1) - 1).astype(jnp.int32)
    position = jnp.sum(one_hot * ranking, axis=2).astype(jnp.int32)
    source_ids = jnp.broadcast_to(jnp.arange(N_EP, dtype=jnp.int32)[:, None], (N_EP, pair_count))
    pair_token = slot_token[block_routes, source_ids, position]
    token_part = jnp.sum(pair_token.reshape(TOKENS, TOP, D), axis=1)
    gate_grad = slot_gate[block_routes, source_ids, position].reshape(TOKENS, TOP)
    weights_f = gate_weights.astype(jnp.float32)
    mixed_term = jnp.sum(weights_f * gate_grad, axis=1, keepdims=True)
    logit_grad = weights_f * (gate_grad - mixed_term)
    signal = jnp.sum(jnp.where(routing[:, :, None] == labels[None, None, :], logit_grad[:, :, None], jnp.float32(0.0)), axis=1).astype(jnp.bfloat16)
    router_grad = jnp.dot(signal.T, tokens, preferred_element_type=jnp.float32)
    token_grad = token_part + jnp.dot(signal, router.T, preferred_element_type=jnp.float32)
    return (token_grad, gate_grad, gate_grads, up_grads, down_grads, router_grad, gate_square, up_square, down_square)
```

```python
import functools

import jax
import jax.numpy as jnp
from jax import lax
from jax.experimental import pallas as pl
from jax.experimental.pallas import tpu as pltpu
from jax.sharding import PartitionSpec as P

LANE = 128
META = 16
BF = jnp.bfloat16
F32 = jnp.float32
MIB = 1024 * 1024


def matmul_tn(left_side, right_side):
    return lax.dot_general(
        left_side, right_side, (((0,), (0,)), ((), ())), preferred_element_type=jnp.float32
    )


def matmul_nt(left_side, right_side):
    return lax.dot_general(
        left_side, right_side, (((1,), (1,)), ((), ())), preferred_element_type=jnp.float32
    )


def slot_table(routing, experts, capacity):
    flat_routes = routing.reshape(-1)
    labels = lax.broadcasted_iota(jnp.int32, (flat_routes.shape[0], experts), 1)
    hit_mask = (flat_routes[:, None] == labels).astype(jnp.int32)
    ranking = jnp.cumsum(hit_mask, axis=0) - 1
    position = jnp.sum(hit_mask * ranking, axis=1)
    slot_id = flat_routes * capacity + position
    slot_index = lax.broadcasted_iota(jnp.int32, (experts * capacity, flat_routes.shape[0]), 0)
    return slot_index == slot_id[None, :]


def generic_shards(tokens, routing, gate_weights, cotangent, expert_gate, expert_up, expert_down, router):
    tok_rows, local_width = tokens.shape
    top_count = routing.shape[1]
    experts = router.shape[1]
    n_tp = lax.axis_size("tp")
    capacity = 3 * top_count * tok_rows // (2 * experts)
    slot_count = experts * capacity
    matches = slot_table(routing, experts, capacity)
    by_token = jnp.any(matches.reshape(slot_count, tok_rows, top_count), axis=2).astype(
        jnp.bfloat16
    )
    input_send = jnp.dot(by_token, tokens, preferred_element_type=jnp.float32).astype(jnp.bfloat16)
    tangent_send = jnp.dot(by_token, cotangent, preferred_element_type=jnp.float32).astype(
        jnp.bfloat16
    )
    weight_flat = gate_weights.reshape(-1).astype(jnp.float32)
    weight_send = jnp.sum(jnp.where(matches, weight_flat[None, :], 0.0), axis=1).astype(
        jnp.bfloat16
    )
    input_slots, tangent_slots, weight_slots = (
        lax.all_to_all(
            input_send.reshape(experts, capacity, local_width),
            "ep",
            split_axis=0,
            concat_axis=0,
            tiled=True,
        ),
        lax.all_to_all(
            tangent_send.reshape(experts, capacity, local_width),
            "ep",
            split_axis=0,
            concat_axis=0,
            tiled=True,
        ),
        lax.all_to_all(
            weight_send.reshape(experts, capacity), "ep", split_axis=0, concat_axis=0, tiled=True
        ),
    )
    input_slots = input_slots.reshape(slot_count, local_width)
    tangent_slots = tangent_slots.reshape(slot_count, local_width)
    slot_weight = weight_slots.reshape(slot_count, 1).astype(jnp.float32)
    gate_matrix = expert_gate[0]
    up_matrix = expert_up[0]
    down_matrix = expert_down[0]
    hidden_local = gate_matrix.shape[1]
    full_input, full_tangent = (
        lax.all_gather(input_slots, "tp", axis=1, tiled=True),
        lax.all_gather(tangent_slots, "tp", axis=1, tiled=True),
    )
    pre_gate = jnp.dot(full_input, gate_matrix, preferred_element_type=jnp.float32)
    pre_up = jnp.dot(full_input, up_matrix, preferred_element_type=jnp.float32)
    back_proj = matmul_nt(full_tangent, down_matrix)
    sigmoid_gate = jax.nn.sigmoid(pre_gate)
    active = pre_gate * sigmoid_gate
    hidden = active * pre_up
    slot_part = jnp.sum(hidden * back_proj, axis=1)
    scaled = (slot_weight * hidden).astype(jnp.bfloat16)
    hidden_grad = slot_weight * back_proj
    gate_pre_grad = (
        hidden_grad * pre_up * sigmoid_gate * (1.0 + pre_gate * (1.0 - sigmoid_gate))
    ).astype(jnp.bfloat16)
    up_pre_grad = (hidden_grad * active).astype(jnp.bfloat16)
    gate_sum = matmul_tn(full_input, gate_pre_grad)
    up_sum = matmul_tn(full_input, up_pre_grad)
    down_sum = matmul_tn(scaled, full_tangent)
    unit_count = hidden_local * n_tp
    slot_gate_grad, gate_square, up_square = lax.psum(
        (slot_part, jnp.sum(gate_sum * gate_sum, axis=1), jnp.sum(up_sum * up_sum, axis=1)), "tp"
    )
    slot_grad = lax.psum_scatter(
        (matmul_nt(gate_matrix, gate_pre_grad) + matmul_nt(up_matrix, up_pre_grad)).astype(
            jnp.bfloat16
        ),
        "tp",
        scatter_dimension=0,
        tiled=True,
    ).astype(jnp.float32)
    back_rows, back_gate = (
        lax.all_to_all(
            slot_grad.reshape(local_width, experts, capacity).astype(jnp.bfloat16),
            "ep",
            split_axis=1,
            concat_axis=1,
            tiled=True,
        ).astype(jnp.float32),
        lax.all_to_all(
            slot_gate_grad.reshape(1, experts, capacity).astype(jnp.bfloat16),
            "ep",
            split_axis=1,
            concat_axis=1,
            tiled=True,
        ).astype(jnp.float32),
    )
    back_flat = back_rows.reshape(local_width, slot_count)
    token_part = lax.dot_general(
        by_token.astype(jnp.float32),
        back_flat,
        (((0,), (1,)), ((), ())),
        precision=lax.Precision.HIGHEST,
        preferred_element_type=jnp.float32,
    )
    gate_grad = jnp.sum(jnp.where(matches, back_gate.reshape(slot_count, 1), 0.0), axis=0).reshape(
        tok_rows, top_count
    )
    weights_f = gate_weights.astype(jnp.float32)
    mixed_term = jnp.sum(weights_f * gate_grad, axis=1, keepdims=True)
    logit_grad = weights_f * (gate_grad - mixed_term)
    labels = lax.broadcasted_iota(jnp.int32, (1, 1, experts), 2)
    signal = jnp.sum(
        jnp.where(routing[:, :, None] == labels, logit_grad[:, :, None], 0.0), axis=1
    ).astype(jnp.bfloat16)
    router_term = matmul_tn(signal, tokens)
    router_grad = lax.psum_scatter(router_term, "ep", scatter_dimension=0, tiled=True)
    router_cols = lax.dynamic_slice_in_dim(
        router, lax.axis_index("tp") * local_width, local_width, 0
    )
    token_grad = token_part + matmul_nt(signal, router_cols)
    return (
        token_grad,
        gate_grad,
        gate_sum.astype(jnp.bfloat16)[None],
        up_sum.astype(jnp.bfloat16)[None],
        down_sum.astype(jnp.bfloat16)[None],
        router_grad,
        (gate_square / unit_count)[None, :],
        (up_square / unit_count)[None, :],
        jnp.mean(down_sum * down_sum, axis=1)[None, :],
    )


def mm(a, b):
    return jnp.dot(a, b, preferred_element_type=F32)


def iota(shape, dim):
    return lax.broadcasted_iota(jnp.int32, shape, dim)


def one_hot_eye(rows):
    return (iota((rows, LANE), 0) == iota((rows, LANE), 1)).astype(BF)


def full(shape):
    zeros = (0,) * len(shape)
    return pl.BlockSpec(shape, lambda *_: zeros)


def split_pair(value):
    high = value.astype(BF).astype(F32)
    return high, value - high


def slots_kernel(cap, route_ref, weight_ref, token_ref, tangent_ref, match_ref, *send_refs):
    experts = len(send_refs)
    tok_rows, width = token_ref.shape
    own = lax.axis_index("ep")
    first, second = route_ref[0:1, :], route_ref[1:2, :]
    weights = weight_ref[...].astype(F32)
    w_first, w_second = weights[0:1, :], weights[1:2, :]
    labels = iota((experts, tok_rows), 0) ^ own
    hit_first, hit_second = labels == first, labels == second
    hit = jnp.logical_or(hit_first, hit_second)
    earlier = (iota((tok_rows, tok_rows), 0) < iota((tok_rows, tok_rows), 1)).astype(BF)
    rank = mm(hit.astype(BF), earlier)
    rank = jnp.where(hit, rank, -1.0).astype(jnp.int32)
    places = iota((LANE, tok_rows), 0)
    padded = [(places == rank[k : k + 1, :]).astype(BF) for k in range(experts)]
    match = jnp.concatenate([part[:cap] for part in padded], axis=0)
    match_ref[...] = match
    rows = mm(match, token_ref[...]).astype(BF)
    cots = mm(match, tangent_ref[...]).astype(BF)
    own_weight = jnp.where(hit_first, w_first, w_second)
    other_weight = jnp.where(hit_first, w_second, w_first)
    other_label = jnp.where(hit_first, second, first).astype(F32)
    line = iota((META, tok_rows), 0)
    chunks = width // LANE
    for k, ref in enumerate(send_refs):
        for c in range(chunks):
            block = (slice(k * cap, (k + 1) * cap), slice(c * LANE, (c + 1) * LANE))
            ref[c * cap : (c + 1) * cap, :] = rows[block]
            ref[(chunks + c) * cap : (chunks + c + 1) * cap, :] = cots[block]
        meta = jnp.where(
            line == 0,
            own_weight[k : k + 1, :],
            jnp.where(
                line == 1,
                other_weight[k : k + 1, :],
                jnp.where(line == 2, other_label[k : k + 1, :], 0.0),
            ),
        )
        ref[2 * chunks * cap :, :] = matmul_nt(meta.astype(BF), padded[k]).astype(BF)


def expert_kernel(
    cap,
    own_ref,
    core_ref,
    far_ref,
    both_ref,
    gate_ref,
    up_ref,
    down_ref,
    rows_ref,
    cots_ref,
    gate_grad_ref,
    up_grad_ref,
    scaled_ref,
    keep_ref,
    send_ref,
    total_ref,
    weight_ref,
    part_ref,
):
    step, steps = pl.program_id(0), pl.num_programs(0)
    own = lax.axis_index("tp")
    blocks = own_ref.shape[0]
    slots, width = rows_ref.shape
    local = width // 4
    chunks = local // LANE

    def place(q):
        return pl.multiple_of((own ^ q) * local, local)

    @pl.when(step == 0)
    def _():
        eye = one_hot_eye(cap)
        for q, ref in enumerate((own_ref, core_ref, far_ref, both_ref)):
            for b in range(blocks):
                for base, dst in ((0, rows_ref), (chunks, cots_ref)):
                    piece = jnp.concatenate(
                        [
                            ref[b, (base + c) * cap : (base + c + 1) * cap, :]
                            for c in range(chunks)
                        ],
                        axis=1,
                    )
                    dst[b * cap : (b + 1) * cap, pl.ds(place(q), local)] = piece
        for b in range(blocks):
            meta = own_ref[b, 2 * chunks * cap :, :]
            column = matmul_nt(eye, meta)[:, 0:1]
            weight_ref[b * cap : (b + 1) * cap, :] = jnp.broadcast_to(column, (cap, LANE))
        total_ref[...] = jnp.zeros_like(total_ref)
        part_ref[...] = jnp.zeros_like(part_ref)

    gate, up = gate_ref[...], up_ref[...]
    pre_gate = mm(rows_ref[...], gate)
    pre_up = mm(rows_ref[...], up)
    back = matmul_nt(cots_ref[...], down_ref[...])
    weight = weight_ref[:, 0:1]
    sigmoid_gate = jax.nn.sigmoid(pre_gate)
    active = pre_gate * sigmoid_gate
    hidden = active * pre_up
    part_ref[...] += jnp.sum(hidden * back, axis=1, keepdims=True)
    scaled_ref[...] = (weight * hidden).astype(BF)
    hidden_grad = weight * back
    gate_pre = (
        hidden_grad * pre_up * sigmoid_gate * (1.0 + pre_gate * (1.0 - sigmoid_gate))
    ).astype(BF)
    up_pre = (hidden_grad * active).astype(BF)
    gate_grad_ref[...] = gate_pre
    up_grad_ref[...] = up_pre
    total_ref[...] += matmul_nt(gate_pre, gate) + matmul_nt(up_pre, up)

    @pl.when(step == steps - 1)
    def _():
        eye = one_hot_eye(cap)
        high, low = split_pair(part_ref[...])
        lane = iota((slots, LANE), 1)
        pair = jnp.where(lane == 0, high, jnp.where(lane == 1, low, 0.0)).astype(BF)
        for b in range(blocks):
            lines = matmul_tn(pair[b * cap : (b + 1) * cap, :], eye)[:META].astype(BF)
            for n, dst in ((0, keep_ref), (1, keep_ref), (0, send_ref), (1, send_ref)):
                dst[n, b, chunks * cap :, :] = lines
        for q, dst, n in ((0, keep_ref, 0), (2, keep_ref, 1), (1, send_ref, 0), (3, send_ref, 1)):
            piece = total_ref[:, pl.ds(place(q), local)].astype(BF)
            for b in range(blocks):
                for c in range(chunks):
                    dst[n, b, c * cap : (c + 1) * cap, :] = piece[
                        b * cap : (b + 1) * cap, c * LANE : (c + 1) * LANE
                    ]


def paired_lines(first, second):
    total = first[0:1] + first[1:2] + second[0:1] + second[1:2]
    high, low = split_pair(total)
    line = iota((META, LANE), 0)
    return total, jnp.where(line == 0, high, jnp.where(line == 1, low, 0.0))


def core_sum_kernel(keep_ref, got_ref, mine_ref, send_ref):
    blocks, rows, _ = mine_ref.shape
    last = rows - META
    for n, dst in ((1, send_ref), (0, mine_ref)):
        summed = keep_ref[n, :, :last, :].astype(F32) + got_ref[n, :, :last, :].astype(F32)
        dst[:, :last, :] = summed.astype(dst.dtype)
        for b in range(blocks):
            lines = paired_lines(
                keep_ref[n, b, last:, :].astype(F32), got_ref[n, b, last:, :].astype(F32)
            )[1]
            dst[b, last:, :] = lines.astype(dst.dtype)


def return_kernel(cap, mine_a, got_a, own_a, mine_b, got_b, own_b, *out_refs):
    experts = len(out_refs)
    own = lax.axis_index("ep")
    half = experts // 2
    last = mine_a.shape[1] - META
    chunks = last // cap
    local = chunks * LANE
    labels = iota((experts, LANE), 0)
    rows_total = jnp.zeros((2 * experts, local), F32)
    lines = []
    for k, ref in enumerate(out_refs):
        mine, got, data = (mine_a, got_a, own_a) if k < half else (mine_b, got_b, own_b)
        b = k % half
        ref[:last, :] = (mine[b, :last, :] + got[b, :last, :].astype(F32)).astype(BF)
        total, pair = paired_lines(mine[b, last:, :], got[b, last:, :].astype(F32))
        lines.append(pair)
        meta = data[b, 2 * last :, :].astype(F32)
        weight, other, label = meta[0:1], meta[1:2], meta[2:3].astype(jnp.int32)
        same = weight * (1.0 - weight) * total
        cross = -(weight * other) * total
        coef = jnp.where(
            labels == 0, same, jnp.where((labels ^ own) == label, cross, 0.0)
        )
        high, low = split_pair(coef)
        coef_pair = jnp.concatenate([high, low], axis=0).astype(BF)[:, :cap]
        tokens = jnp.concatenate(
            [data[b, c * cap : (c + 1) * cap, :] for c in range(chunks)], axis=1
        )
        rows_total += mm(coef_pair, tokens)
    router_rows = rows_total[:experts] + rows_total[experts:]
    line = iota((META, LANE), 0)
    for k, ref in enumerate(out_refs):
        block = lines[k]
        for c in range(chunks):
            high, low = split_pair(router_rows[k : k + 1, c * LANE : (c + 1) * LANE])
            block = jnp.where(
                line == 2 + c, high, jnp.where(line == 2 + chunks + c, low, block)
            )
        ref[last:, :] = block.astype(BF)


def combine_kernel(cap, match_ref, route_ref, weight_ref, router_ref, *refs):
    back_refs, (token_ref, gate_ref, router_grad_ref) = refs[:-3], refs[-3:]
    experts = len(back_refs)
    tok_rows, local = token_ref.shape
    chunks = local // LANE
    last = chunks * cap
    own = lax.axis_index("ep")
    blocks, gates = [], []
    router_lines = jnp.zeros((META, LANE), F32)
    for k, ref in enumerate(back_refs):
        blocks.append(
            jnp.concatenate([ref[c * cap : (c + 1) * cap, :] for c in range(chunks)], axis=1)
        )
        lines = ref[last:, :]
        spread = mm(lines[:, :cap], match_ref[k * cap : (k + 1) * cap, :])
        gates.append(spread[0:1] + spread[1:2])
        router_lines += lines.astype(F32)
    for c in range(chunks):
        router_grad_ref[:, c * LANE : (c + 1) * LANE] = (
            router_lines[2 + c : 3 + c] + router_lines[2 + chunks + c : 3 + chunks + c]
        )
    token_part = matmul_tn(match_ref[...], jnp.concatenate(blocks, axis=0))
    slot_gates = jnp.concatenate(gates, axis=0)
    first, second = route_ref[0:1, :], route_ref[1:2, :]
    labels = iota((experts, tok_rows), 0)
    places = labels ^ own
    gate_first = jnp.sum(jnp.where(places == first, slot_gates, 0.0), axis=0, keepdims=True)
    gate_second = jnp.sum(jnp.where(places == second, slot_gates, 0.0), axis=0, keepdims=True)
    gate_ref[...] = jnp.concatenate([gate_first, gate_second], axis=0)
    weights = weight_ref[...].astype(F32)
    w_first, w_second = weights[0:1, :], weights[1:2, :]
    mixed = w_first * gate_first + w_second * gate_second
    signal = (
        jnp.where(labels == first, w_first * (gate_first - mixed), 0.0)
        + jnp.where(labels == second, w_second * (gate_second - mixed), 0.0)
    ).astype(BF)
    token_ref[...] = token_part + matmul_tn(signal, router_ref[...])


def input_grad_kernel(rows_a, rows_b, gate_a, gate_b, up_a, up_b, gate_ref, up_ref, square_ref):
    left_a, left_b = rows_a[...], rows_b[...]
    width = square_ref.shape[1]
    for n, (part_a, part_b, dst) in enumerate(((gate_a, gate_b, gate_ref), (up_a, up_b, up_ref))):
        total = matmul_tn(left_a, part_a[...]) + matmul_tn(left_b, part_b[...])
        dst[0] = total.astype(BF)
        column = jnp.sum(total * total, axis=1, keepdims=True)
        square_ref[n : n + 1, :] = jnp.transpose(jnp.broadcast_to(column, (width, LANE)))[0:1, :]


def down_grad_kernel(scaled_a, scaled_b, cots_a, cots_b, down_ref, square_ref, part_ref):
    step, steps = pl.program_id(0), pl.num_programs(0)
    total = matmul_tn(scaled_a[...], cots_a[...]) + matmul_tn(scaled_b[...], cots_b[...])
    down_ref[0] = total.astype(BF)
    column = jnp.sum(total * total, axis=1, keepdims=True)

    @pl.when(step == 0)
    def _():
        part_ref[...] = jnp.zeros_like(part_ref)

    part_ref[...] += column

    @pl.when(step == steps - 1)
    def _():
        full_width = steps * cots_a.shape[1]
        square_ref[...] = jnp.transpose(part_ref[...])[0:1, :] * (1.0 / full_width)


def swap(value, axis, distance):
    size = lax.axis_size(axis)
    return lax.ppermute(value, axis, [(n, n ^ distance) for n in range(size)])


def shards(tokens, routing, gate_weights, cotangent, expert_gate, expert_up, expert_down, router):
    tok_rows, local = tokens.shape
    top_count = routing.shape[1]
    experts = router.shape[1]
    n_tp = lax.axis_size("tp")
    cap = 3 * top_count * tok_rows // (2 * experts)
    width = local * n_tp
    hidden_local = expert_gate.shape[2]
    half = experts // 2
    slots = half * cap
    chunks = local // LANE
    sent_rows = 2 * chunks * cap + META
    back_rows = chunks * cap + META
    gate_matrix, up_matrix, down_matrix = expert_gate[0], expert_up[0], expert_down[0]
    routes, weights = routing.T, gate_weights.T
    sds = jax.ShapeDtypeStruct
    router_cols = lax.dynamic_slice_in_dim(router.T, lax.axis_index("tp") * local, local, 1)

    built = pl.pallas_call(
        functools.partial(slots_kernel, cap),
        out_shape=[sds((experts * cap, tok_rows), BF)] + [sds((sent_rows, LANE), BF)] * experts,
        name="slots",
    )(routes, weights, tokens, cotangent)
    match, sends = built[0], built[1:]
    order = list(range(half, experts)) + list(range(1, half))
    got = {0: sends[0]}
    for k in order:
        got[k] = swap(sends[k], "ep", k)

    block_step = 256
    steps = hidden_local // block_step
    results = []
    for side in range(2):
        own = jnp.stack([got[side * half + b] for b in range(half)])
        far = swap(own, "tp", 2)
        core = swap(own, "tp", 1)
        both = swap(far, "tp", 1)
        sent = (half, sent_rows, LANE)
        back = (2, half, back_rows, LANE)
        (rows, cots, gate_pre, up_pre, scaled, keep, send) = pl.pallas_call(
            functools.partial(expert_kernel, cap),
            grid=(steps,),
            in_specs=[full(sent)] * 4
            + [
                pl.BlockSpec((width, block_step), lambda f: (0, f)),
                pl.BlockSpec((width, block_step), lambda f: (0, f)),
                pl.BlockSpec((block_step, width), lambda f: (f, 0)),
            ],
            out_specs=[full((slots, width))] * 2
            + [pl.BlockSpec((slots, block_step), lambda f: (0, f))] * 3
            + [full(back)] * 2,
            out_shape=[sds((slots, width), BF)] * 2
            + [sds((slots, hidden_local), BF)] * 3
            + [sds(back, BF)] * 2,
            scratch_shapes=[
                pltpu.VMEM((slots, width), F32),
                pltpu.VMEM((slots, LANE), F32),
                pltpu.VMEM((slots, LANE), F32),
            ],
            compiler_params=pltpu.CompilerParams(vmem_limit_bytes=32 * MIB),
            name=f"expert{side}",
        )(own, core, far, both, gate_matrix, up_matrix, down_matrix)
        taken = swap(send, "tp", 1)
        mine, onward = pl.pallas_call(
            core_sum_kernel,
            out_shape=[sds((half, back_rows, LANE), F32), sds((half, back_rows, LANE), BF)],
            name=f"coresum{side}",
        )(keep, taken)
        arrived = swap(onward, "tp", 2)
        results.append((rows, cots, gate_pre, up_pre, scaled, mine, arrived, own))

    (rows_a, cots_a, gate_a, up_a, scaled_a, mine_a, arrived_a, own_a) = results[0]
    (rows_b, cots_b, gate_b, up_b, scaled_b, mine_b, arrived_b, own_b) = results[1]
    feature_step = local
    gate_sum, up_sum, squares = pl.pallas_call(
        input_grad_kernel,
        grid=(width // feature_step,),
        in_specs=[pl.BlockSpec((slots, feature_step), lambda f: (0, f))] * 2
        + [full((slots, hidden_local))] * 4,
        out_specs=[pl.BlockSpec((1, feature_step, hidden_local), lambda f: (0, f, 0))] * 2
        + [pl.BlockSpec((2, feature_step), lambda f: (0, f))],
        out_shape=[sds((1, width, hidden_local), BF)] * 2 + [sds((2, width), F32)],
        compiler_params=pltpu.CompilerParams(vmem_limit_bytes=32 * MIB),
        name="inputgrad",
    )(rows_a, rows_b, gate_a, gate_b, up_a, up_b)
    returns = pl.pallas_call(
        functools.partial(return_kernel, cap),
        out_shape=[sds((back_rows, LANE), BF)] * experts,
        name="returns",
    )(mine_a, arrived_a, own_a, mine_b, arrived_b, own_b)
    home = {0: returns[0]}
    for k in order:
        home[k] = swap(returns[k], "ep", k)
    squares = squares + swap(squares, "tp", 1)
    squares = squares + swap(squares, "tp", 2)
    down_sum, down_square = pl.pallas_call(
        down_grad_kernel,
        grid=(width // feature_step,),
        in_specs=[full((slots, hidden_local))] * 2
        + [pl.BlockSpec((slots, feature_step), lambda f: (0, f))] * 2,
        out_specs=[
            pl.BlockSpec((1, hidden_local, feature_step), lambda f: (0, 0, f)),
            full((1, hidden_local)),
        ],
        out_shape=[sds((1, hidden_local, width), BF), sds((1, hidden_local), F32)],
        scratch_shapes=[pltpu.VMEM((hidden_local, LANE), F32)],
        compiler_params=pltpu.CompilerParams(vmem_limit_bytes=32 * MIB),
        name="downgrad",
    )(scaled_a, scaled_b, cots_a, cots_b)
    token_grad, gate_grad, router_grad = pl.pallas_call(
        functools.partial(combine_kernel, cap),
        out_shape=[sds((tok_rows, local), F32), sds((2, tok_rows), F32), sds((1, local), F32)],
        name="combine",
    )(match, routes, weights, router_cols, *[home[k] for k in range(experts)])
    unit_count = hidden_local * n_tp
    squares = squares * (1.0 / unit_count)
    return (
        token_grad,
        gate_grad.T,
        gate_sum,
        up_sum,
        down_sum,
        router_grad,
        squares[0:1],
        squares[1:2],
        down_square,
    )


def paired_layout(mesh, tokens, routing, expert_gate, router):
    n_ep, n_tp = mesh.shape["ep"], mesh.shape["tp"]
    tok_rows, local = tokens.shape[0] // n_ep, tokens.shape[1] // n_tp
    experts = router.shape[1]
    cap = 3 * routing.shape[1] * tok_rows // (2 * experts)
    return (
        n_tp == 4
        and n_ep == experts
        and n_ep in (4, 8, 16)
        and routing.shape[1] == 2
        and tok_rows == LANE
        and cap % 16 == 0
        and local % LANE == 0
        and 2 + 2 * (local // LANE) <= META
        and (expert_gate.shape[2] // n_tp) % 256 == 0
    )


def solution(mesh):
    in_specs = (
        P("ep", "tp"),
        P("ep", None),
        P("ep", None),
        P("ep", "tp"),
        P("ep", None, "tp"),
        P("ep", None, "tp"),
        P("ep", "tp", None),
        P(),
    )
    out_specs = (
        P("ep", "tp"),
        P("ep", None),
        P("ep", None, "tp"),
        P("ep", None, "tp"),
        P("ep", "tp", None),
        P("ep", "tp"),
        P("ep", None),
        P("ep", None),
        P("ep", "tp"),
    )

    def run(*args):
        fits = paired_layout(mesh, args[0], args[1], args[4], args[7])
        body = shards if fits else generic_shards
        return jax.shard_map(
            body, mesh=mesh, in_specs=in_specs, out_specs=out_specs, check_vma=False
        )(*args)

    return run
```
